32 devices in a mesh: dp: 4 (over y, x), kv: 4 (over z), tp: 2 (over core).
Axes of the slice: x: 2, y: 2, z: 4, core: 2. Of those that a mesh axis runs over, the one named last changes fastest.
Arguments:
- tokens: bfloat16 [4, 3072, 2048], P('dp', 'kv'), may hold values from -60 to 60
- query_weight: bfloat16 [2048, 1024], P(None, 'tp'), may hold values from -0.125 to 0.125
- key_weight: bfloat16 [2048, 256], P(None, 'tp'), may hold values from -0.125 to 0.125
- value_weight: bfloat16 [2048, 256], P(None, 'tp'), may hold values from -0.125 to 0.125
- out_weight: bfloat16 [1024, 2048], P('tp'), may hold values from -3 to 3
- norm_gain: float32 [2048], P('tp'), may hold values from 0.1 to 1.9
- chosen_owner: int32 [4, 24, 4], P('dp'), may hold values from -1 to 3, as said below
- chosen_part: int32 [4, 24, 4], P('dp'), may hold values from 0 to 11, as said below
Outputs:
- attended: bfloat16 [4, 3072, 2048], P('dp', 'kv', 'tp')
The draws below stay inside these ranges and needn't reach their ends.
Inputs may be any that keep to these rules, and one draw needn't show every extreme that they name: `chosen_owner`: within a row the indices other than -1 are different. Every named key block lies wholly before its query block's first position. Among the 6 rows of one index of kv, no index is named by more than 6 rows. `chosen_part`: 0 where the owner is -1.
All inputs are finite; a program needn't handle non-finite values.
Results may differ from the reference program's by a relative error of at most 0.014.
The reference program's roundings to bfloat16 on the way count: a program that leaves them out, or rounds other values in their place, can miss the bound.
Values may be sent and summed in bfloat16 or wider, within the bound.
A program may use at most 128 MiB of HBM per device.

```python
import jax
import jax.numpy as jnp
from jax import lax

D = 2048
HEADS = 16
KV_HEADS = 4
HEAD_DIM = 64
QUERY_BLOCK = 128
KEY_BLOCK = 64
SEQS = 4
SEQ = 3072
QBLOCKS = 24
QBLOCKS_DEV = 6
KBLOCKS_DEV = 12
CHOSEN = 4
N_KV = 4
N_TP = 2


def draw_tokens(key, part):
    base = jax.random.normal(jax.random.fold_in(key, 11), (SEQS, SEQ, D), jnp.float32)
    base = jnp.clip(base, -6.0, 6.0)
    return base.astype(jnp.bfloat16)


def draw_out_weight(key, part):
    base = jax.random.normal(jax.random.fold_in(key, 21), (HEADS * HEAD_DIM, D), jnp.float32)
    base = jnp.clip(base, -6.0, 6.0) * (HEADS * HEAD_DIM) ** (-0.5)
    column = jnp.arange(D, dtype=jnp.float32) / D
    jitter = jnp.exp(jax.random.uniform(jax.random.fold_in(key, 22), (D,), jnp.float32, -0.5, 0.5))
    rising = 3.0 ** column
    return (base * (rising * jitter)[None, :] * 0.5).astype(jnp.bfloat16)


def chosen_pair(key):
    block_ids = jnp.arange(QBLOCKS, dtype=jnp.int32)
    device_ids = block_ids // QBLOCKS_DEV
    local_ids = block_ids % QBLOCKS_DEV
    owners = jnp.arange(N_KV, dtype=jnp.int32)
    earlier = owners[None, :] < device_ids[:, None]
    itself = jnp.logical_and(owners[None, :] == device_ids[:, None], local_ids[:, None] > 0)
    allowed = jnp.logical_or(earlier, itself)
    forced = jnp.logical_or(jnp.logical_or(owners[None, :] == 0, owners[None, :] == device_ids[:, None] - 1), jnp.logical_or(owners[None, :] == device_ids[:, None] - N_KV // 2, owners[None, :] == device_ids[:, None]))
    forced = jnp.logical_and(forced, allowed)
    noise = jax.random.randint(jax.random.fold_in(key, 31), (SEQS, QBLOCKS, N_KV), 0, 16384)
    scores = noise + (N_KV - owners)[None, None, :] * (16384 // N_KV) + forced[None].astype(jnp.int32) * 1048576
    scores = jnp.where(allowed[None], scores, -2097152)
    scores = scores * 64 + owners[None, None, :]
    picked = lax.top_k(scores, CHOSEN)[1].astype(jnp.int32)
    valid = jnp.take_along_axis(jnp.broadcast_to(allowed[None], (SEQS, QBLOCKS, N_KV)), picked, axis=2)
    owner_out = jnp.where(valid, picked, -1).astype(jnp.int32)
    limit = jnp.where(picked == device_ids[None, :, None], QUERY_BLOCK // KEY_BLOCK * local_ids[None, :, None], KBLOCKS_DEV)
    limit = jnp.maximum(limit, 1)
    raw_part = jax.random.randint(jax.random.fold_in(key, 32), (SEQS, QBLOCKS, CHOSEN), 0, 1048576)
    part_out = jnp.where(valid, raw_part % limit, 0).astype(jnp.int32)
    return (owner_out, part_out)


def draw_chosen_owner(key, part):
    return chosen_pair(jax.random.fold_in(key, 41))[0]


def draw_chosen_part(key, part):
    return chosen_pair(jax.random.fold_in(key, 41))[1]


def level_of(own_key, dims, cuts, least, high):
    gain, own = 1.0, jax.random.fold_in(own_key, 6)
    for axis_at, parts in cuts:
        draws = jnp.exp(jax.random.uniform(jax.random.fold_in(own, axis_at), (parts,), jnp.float32, least / len(cuts), high / len(cuts)))
        gain = gain * jnp.repeat(draws, dims[axis_at] // parts).reshape([-1 if axis == axis_at else 1 for axis in range(len(dims))])
    return gain


def bell_draw(rng, shape, deviation, bound, split=(), held_as=jnp.bfloat16):
    factor_of = level_of(rng, shape, split, -0.22, 0.18) if split else 1.0
    drawn = jax.random.normal(rng, shape, jnp.float32) * deviation * factor_of
    return jnp.minimum(jnp.maximum(drawn, -bound), bound).astype(held_as)


def setup_inputs(seed: int = 0) -> dict:
    keys = jax.random.split(jax.random.key(seed), 9)
    tokens = draw_tokens(jax.random.fold_in(keys[8], 71), 0)
    query_weight = bell_draw(keys[1], (D, HEADS * HEAD_DIM), D ** -0.5, 0.125, ((1, 2),))
    key_weight = bell_draw(keys[2], (D, KV_HEADS * HEAD_DIM), D ** -0.5, 0.125, ((1, 2),))
    value_weight = bell_draw(keys[3], (D, KV_HEADS * HEAD_DIM), D ** -0.5, 0.125, ((1, 2),))
    out_weight = draw_out_weight(jax.random.fold_in(keys[8], 71), 0)
    norm_gain = jnp.clip(1.0 + 0.18 * jax.random.normal(keys[5], (D,), jnp.float32), 0.1, 1.9)
    chosen_owner = draw_chosen_owner(jax.random.fold_in(keys[8], 71), 0)
    chosen_part = draw_chosen_part(jax.random.fold_in(keys[8], 71), 0)
    return {"tokens": tokens, "query_weight": query_weight, "key_weight": key_weight, "value_weight": value_weight, "out_weight": out_weight, "norm_gain": norm_gain, "chosen_owner": chosen_owner, "chosen_part": chosen_part}


rope_base = 10000.0
norm_eps = 1e-06

def rotate(head_rows, positions):
    half_dim = head_rows.shape[-1] // 2
    frequency = rope_base ** (-jnp.arange(half_dim, dtype=jnp.float32) / half_dim)
    angles = positions.astype(jnp.float32)[:, None] * frequency
    cosine = jnp.cos(angles)[:, None, :]
    sine_part = jnp.sin(angles)[:, None, :]
    first_half = head_rows[..., :half_dim]
    second_half = head_rows[..., half_dim:]
    return jnp.concatenate([first_half * cosine - second_half * sine_part, second_half * cosine + first_half * sine_part], axis=-1)

def reference(tokens, query_weight, key_weight, value_weight, out_weight, norm_gain, chosen_owner, chosen_part):
    group_size = HEADS // KV_HEADS
    lower_mask = jnp.arange(QUERY_BLOCK)[:, None] >= jnp.arange(QUERY_BLOCK)[None, :]

    def one_sequence(seq_items):
        row_data, owner_ids, part_ids = seq_items
        positions = jnp.arange(SEQ, dtype=jnp.int32)
        queries = rotate(jnp.dot(row_data, query_weight, preferred_element_type=jnp.float32).reshape(SEQ, HEADS, HEAD_DIM), positions).astype(jnp.bfloat16)
        key_rows = rotate(jnp.dot(row_data, key_weight, preferred_element_type=jnp.float32).reshape(SEQ, KV_HEADS, HEAD_DIM), positions).astype(jnp.bfloat16)
        value_rows = jnp.dot(row_data, value_weight, preferred_element_type=jnp.float32).astype(jnp.bfloat16).reshape(SEQ, KV_HEADS, HEAD_DIM)
        key_blocks = key_rows.reshape(SEQ // KEY_BLOCK, KEY_BLOCK, KV_HEADS, HEAD_DIM)
        value_blocks = value_rows.reshape(SEQ // KEY_BLOCK, KEY_BLOCK, KV_HEADS, HEAD_DIM)
        slot_valid = owner_ids >= 0
        chosen_ids = jnp.where(slot_valid, owner_ids * KBLOCKS_DEV + part_ids, 0).astype(jnp.int32)

        def one_block(block_index):
            block_start = (block_index * QUERY_BLOCK).astype(jnp.int32)
            picked_ids = chosen_ids[block_index]
            valid_row = slot_valid[block_index]
            block_queries = lax.dynamic_slice_in_dim(queries, block_start, QUERY_BLOCK, 0).reshape(QUERY_BLOCK, KV_HEADS, group_size, HEAD_DIM).astype(jnp.float32)
            own_keys = lax.dynamic_slice_in_dim(key_rows, block_start, QUERY_BLOCK, 0)
            own_values = lax.dynamic_slice_in_dim(value_rows, block_start, QUERY_BLOCK, 0)
            chosen_keys = key_blocks[picked_ids].reshape(CHOSEN * KEY_BLOCK, KV_HEADS, HEAD_DIM)
            chosen_values = value_blocks[picked_ids].reshape(CHOSEN * KEY_BLOCK, KV_HEADS, HEAD_DIM)
            all_keys = jnp.concatenate([chosen_keys, own_keys], axis=0).astype(jnp.float32)
            all_values = jnp.concatenate([chosen_values, own_values], axis=0).astype(jnp.float32)
            key_valid = jnp.broadcast_to(valid_row[:, None], (CHOSEN, KEY_BLOCK)).reshape(CHOSEN * KEY_BLOCK)
            far_mask = jnp.broadcast_to(key_valid[None, :], (QUERY_BLOCK, CHOSEN * KEY_BLOCK))
            full_mask = jnp.concatenate([far_mask, lower_mask], axis=1)
            scores = jnp.einsum('qngd,knd->ngqk', block_queries, all_keys) * HEAD_DIM ** (-0.5)
            scores = jnp.where(full_mask[None, None], scores, -jnp.inf)
            row_max = lax.optimization_barrier(jnp.max(scores, axis=-1, keepdims=True))
            weights = jnp.exp(scores - row_max)
            weights = (weights / lax.optimization_barrier(jnp.sum(weights, axis=-1, keepdims=True))).astype(jnp.bfloat16)
            mixed_out = jnp.einsum('ngqk,knd->qngd', weights.astype(jnp.float32), all_values)
            return mixed_out.reshape(QUERY_BLOCK, HEADS * HEAD_DIM).astype(jnp.bfloat16)
        mixed_rows = lax.map(one_block, jnp.arange(QBLOCKS, dtype=jnp.int32)).reshape(SEQ, HEADS * HEAD_DIM)
        share_cols = HEADS * HEAD_DIM // N_TP
        summed = jnp.zeros((SEQ, D), jnp.float32)
        for member in range(N_TP):
            partial_value = jnp.dot(mixed_rows[:, member * share_cols:(member + 1) * share_cols], out_weight[member * share_cols:(member + 1) * share_cols], preferred_element_type=jnp.float32).astype(jnp.bfloat16)
            summed = summed + lax.optimization_barrier(partial_value).astype(jnp.float32)
        mean_sq = lax.optimization_barrier(jnp.mean(summed * summed, axis=1, keepdims=True))
        return (summed * lax.rsqrt(mean_sq + norm_eps) * norm_gain.astype(jnp.float32)).astype(jnp.bfloat16)
    return lax.map(one_sequence, (tokens, chosen_owner, chosen_part))
```

```python
import functools

import jax
import jax.numpy as jnp
from jax import lax
from jax.experimental import pallas as pl
from jax.experimental.pallas import tpu as pltpu
from jax.sharding import PartitionSpec as P

HEAD_DIM = 64
QUERY_BLOCK = 128
KEY_BLOCK = 64
LANES = 128
ROWS = 256
COLS = 256

rope_base = 10000.0
norm_eps = 1e-06
MESH = pl.DeviceIdType.MESH


def turn(u, cosine, sine):
    lane = lax.broadcasted_iota(jnp.int32, u.shape, 1)
    half = HEAD_DIM // 2
    swapped = jnp.where(
        lane % HEAD_DIM < half, pltpu.roll(u, LANES - half, 1), pltpu.roll(u, half, 1)
    )
    return u * cosine + swapped * sine


def spread(pair, head):
    wide = pair.astype(jnp.float32)
    swapped = pltpu.roll(wide, HEAD_DIM, 1)
    low = lax.broadcasted_iota(jnp.int32, wide.shape, 1) < HEAD_DIM
    in_low, in_high = (wide, swapped) if head == 0 else (swapped, wide)
    return jnp.concatenate(
        [jnp.where(low, in_low, 0.0), jnp.where(low, 0.0, in_high)], axis=0
    ).astype(jnp.bfloat16)


def kernel(
    devices, owner_ref, part_ref, tok, wq, wk, wv, ow, gain, cosine, sine, out,
    kv, send, pool, queries, mix, mix_other, ow_other, proj, ss, ss_other,
    kv_send, kv_recv, ow_sems, mix_send, mix_recv, ss_sems,
):
    me = lax.axis_index("kv")
    core = lax.axis_index("tp")
    other = 1 - core
    tokens = tok.shape[0]
    qblocks = tokens // QUERY_BLOCK
    chosen = owner_ref.shape[1]
    half = ow_other.shape[1]
    row_steps = tokens // ROWS
    per_q = QUERY_BLOCK // KEY_BLOCK

    barrier = pltpu.get_barrier_semaphore()

    @pl.loop(0, devices)
    def _(j):
        @pl.when(j != me)
        def _():
            pl.semaphore_signal(barrier, inc=1, device_id={"kv": j}, device_id_type=MESH)

    pl.semaphore_signal(barrier, inc=1, device_id={"tp": other}, device_id_type=MESH)

    @pl.loop(0, row_steps)
    def _(r):
        rows = pl.ds(pl.multiple_of(r * ROWS, ROWS), ROWS)
        both = jnp.dot(
            tok[rows, :],
            jnp.concatenate([wk[...], wv[...]], axis=1),
            preferred_element_type=jnp.float32,
        )
        keys = turn(both[:, :LANES], cosine[rows, :], sine[rows, :])
        joined = jnp.concatenate([keys, both[:, LANES:]], axis=1).astype(jnp.bfloat16)
        blocks = ROWS // KEY_BLOCK
        kv[pl.ds(r * blocks, blocks)] = joined.reshape(blocks, KEY_BLOCK, 2 * LANES)

    pl.semaphore_wait(barrier, devices)

    def wanted(dst, q):
        row = dst * qblocks + q
        return sum(
            jnp.where(owner_ref[row, s] == me, part_ref[row, s], 0) for s in range(chosen)
        )

    def kv_copy(src, dst):
        return pltpu.make_async_remote_copy(
            src_ref=send.at[pl.ds(dst * qblocks, qblocks)],
            dst_ref=pool.at[pl.ds(src * qblocks, qblocks)],
            send_sem=kv_send.at[dst],
            recv_sem=kv_recv.at[src],
            device_id={"kv": dst},
            device_id_type=MESH,
        )

    @pl.loop(0, devices)
    def _(dst):
        @pl.when(dst > me)
        def _():
            for q in range(qblocks):
                send[pl.ds(dst * qblocks + q, 1)] = kv[pl.ds(wanted(dst, q), 1)]
            kv_copy(me, dst).start()

        @pl.when(dst == me)
        def _():
            for q in range(qblocks):
                pool[pl.ds(me * qblocks + q, 1)] = kv[pl.ds(wanted(me, q), 1)]

    ow_copy = pltpu.make_async_remote_copy(
        src_ref=ow.at[:, pl.ds(pl.multiple_of(other * half, half), half)],
        dst_ref=ow_other,
        send_sem=ow_sems.at[0],
        recv_sem=ow_sems.at[1],
        device_id={"tp": other},
        device_id_type=MESH,
    )
    ow_copy.start()

    @pl.loop(0, row_steps)
    def _(r):
        rows = pl.ds(pl.multiple_of(r * ROWS, ROWS), ROWS)
        for c in range(wq.shape[1] // COLS):
            part = jnp.dot(
                tok[rows, :], wq[:, c * COLS : (c + 1) * COLS], preferred_element_type=jnp.float32
            )
            for k in range(COLS // LANES):
                at = c * COLS + k * LANES
                queries[rows, at : at + LANES] = turn(
                    part[:, k * LANES : (k + 1) * LANES], cosine[rows, :], sine[rows, :]
                ).astype(jnp.bfloat16)

    @pl.loop(0, devices)
    def _(src):
        @pl.when(src < me)
        def _():
            kv_copy(src, me).wait_recv()

    kv_heads = wk.shape[1] // HEAD_DIM
    slices = wq.shape[1] // LANES // kv_heads
    key_count = chosen * KEY_BLOCK + QUERY_BLOCK

    def mix_copy(b):
        rows = pl.ds(pl.multiple_of(b * QUERY_BLOCK, QUERY_BLOCK), QUERY_BLOCK)
        return pltpu.make_async_remote_copy(
            src_ref=mix.at[rows],
            dst_ref=mix_other.at[rows],
            send_sem=mix_send.at[b],
            recv_sem=mix_recv.at[b],
            device_id={"tp": other},
            device_id_type=MESH,
        )

    @pl.loop(0, qblocks)
    def _(b):
        row = me * qblocks + b
        rows = pl.ds(pl.multiple_of(b * QUERY_BLOCK, QUERY_BLOCK), QUERY_BLOCK)
        pieces = []
        lane = lax.broadcasted_iota(jnp.int32, (1, chosen * KEY_BLOCK), 1) // KEY_BLOCK
        far = jnp.zeros((1, chosen * KEY_BLOCK), jnp.float32)
        for s in range(chosen):
            owner = owner_ref[row, s]
            at = jnp.where(owner >= 0, owner * qblocks + b, 0)
            pieces.append(pool[pl.ds(at, 1)].reshape(KEY_BLOCK, 2 * LANES))
            far = jnp.where(lane == s, jnp.where(owner >= 0, 0.0, -jnp.inf), far)
        pieces.append(kv[pl.ds(b * per_q, per_q)].reshape(QUERY_BLOCK, 2 * LANES))
        near = jnp.where(
            lax.broadcasted_iota(jnp.int32, (slices * QUERY_BLOCK, QUERY_BLOCK), 0) % QUERY_BLOCK
            >= lax.broadcasted_iota(jnp.int32, (slices * QUERY_BLOCK, QUERY_BLOCK), 1),
            0.0,
            -jnp.inf,
        )
        bias = jnp.concatenate(
            [jnp.broadcast_to(far, (slices * QUERY_BLOCK, chosen * KEY_BLOCK)), near], axis=1
        )
        both = jnp.concatenate(pieces, axis=0)
        for n in range(kv_heads):
            q = jnp.concatenate(
                [
                    queries[rows, (n * slices + m) * LANES : (n * slices + m + 1) * LANES]
                    for m in range(slices)
                ],
                axis=0,
            )
            scores = lax.dot_general(
                q,
                spread(both[:, :LANES], n),
                (((1,), (1,)), ((), ())),
                preferred_element_type=jnp.float32,
            )
            probs = []
            for side in range(2):
                s = scores[:, side * key_count : (side + 1) * key_count] * HEAD_DIM**-0.5 + bias
                e = jnp.exp(s - jnp.max(s, axis=1, keepdims=True))
                probs.append((e * (1.0 / jnp.sum(e, axis=1, keepdims=True))).astype(jnp.bfloat16))
            mixed = jnp.dot(
                jnp.concatenate(probs, axis=1),
                spread(both[:, LANES:], n),
                preferred_element_type=jnp.float32,
            ).astype(jnp.bfloat16)
            for m in range(slices):
                at = (n * slices + m) * LANES
                mix[rows, at : at + LANES] = mixed[m * QUERY_BLOCK : (m + 1) * QUERY_BLOCK]
        mix_copy(b).start()

    ow_copy.wait_recv()

    @pl.loop(0, qblocks)
    def _(b):
        mix_copy(b).wait_recv()

    @pl.loop(0, row_steps)
    def _(r):
        rows = pl.ds(pl.multiple_of(r * ROWS, ROWS), ROWS)
        total = jnp.zeros((ROWS, LANES), jnp.float32)
        for c in range(half // COLS):
            mine = jnp.dot(
                mix[rows, :],
                ow[:, pl.ds(pl.multiple_of(core * half + c * COLS, COLS), COLS)],
                preferred_element_type=jnp.float32,
            ).astype(jnp.bfloat16)
            theirs = jnp.dot(
                mix_other[rows, :],
                ow_other[:, c * COLS : (c + 1) * COLS],
                preferred_element_type=jnp.float32,
            ).astype(jnp.bfloat16)
            added = mine.astype(jnp.float32) + theirs.astype(jnp.float32)
            proj[rows, c * COLS : (c + 1) * COLS] = added
            for k in range(COLS // LANES):
                piece = added[:, k * LANES : (k + 1) * LANES]
                total = total + piece * piece
        for k in range(ROWS // LANES):
            ss[r * (ROWS // LANES) + k] = jnp.sum(
                total[k * LANES : (k + 1) * LANES].T, axis=0, keepdims=True
            )

    ss_copy = pltpu.make_async_remote_copy(
        src_ref=ss,
        dst_ref=ss_other,
        send_sem=ss_sems.at[0],
        recv_sem=ss_sems.at[1],
        device_id={"tp": other},
        device_id_type=MESH,
    )
    ss_copy.start()

    @pl.loop(0, devices)
    def _(dst):
        @pl.when(dst > me)
        def _():
            kv_copy(me, dst).wait_send()

    ow_copy.wait_send()

    @pl.loop(0, qblocks)
    def _(b):
        mix_copy(b).wait_send()

    ss_copy.wait()

    @pl.loop(0, qblocks)
    def _(b):
        rows = pl.ds(pl.multiple_of(b * LANES, LANES), LANES)
        scale = lax.rsqrt((ss[b] + ss_other[b]) / (2 * half) + norm_eps)
        scale = jnp.broadcast_to(scale, (LANES, LANES)).T
        for c in range(half // LANES):
            at = slice(c * LANES, (c + 1) * LANES)
            out[rows, at] = (proj[rows, at] * scale * gain[:, at]).astype(jnp.bfloat16)


def body(
    tokens, query_weight, key_weight, value_weight, out_weight, norm_gain, chosen_owner, chosen_part
):
    row_data = tokens[0]
    count = row_data.shape[0]
    devices = lax.axis_size("kv")
    qblocks = count // QUERY_BLOCK
    positions = lax.axis_index("kv") * count + jnp.arange(count, dtype=jnp.int32)
    half_dim = HEAD_DIM // 2
    frequency = rope_base ** (-jnp.arange(half_dim, dtype=jnp.float32) / half_dim)
    angles = positions.astype(jnp.float32)[:, None] * frequency
    cosine, sine = jnp.cos(angles), jnp.sin(angles)
    cosine = jnp.concatenate([cosine] * (LANES // half_dim), axis=1)
    sine = jnp.concatenate([-sine, sine] * (LANES // HEAD_DIM), axis=1)
    heads_width = query_weight.shape[1]
    half = norm_gain.shape[0]
    vmem = pl.BlockSpec(memory_space=pltpu.VMEM)
    smem = pl.BlockSpec(memory_space=pltpu.SMEM)
    bf16, f32 = jnp.bfloat16, jnp.float32
    result = pl.pallas_call(
        functools.partial(kernel, devices),
        out_shape=jax.ShapeDtypeStruct((count, half), bf16),
        in_specs=[smem] * 2 + [vmem] * 8,
        out_specs=vmem,
        scratch_shapes=[
            pltpu.VMEM((count // KEY_BLOCK, KEY_BLOCK, 2 * LANES), bf16),
            pltpu.VMEM((devices * qblocks, KEY_BLOCK, 2 * LANES), bf16),
            pltpu.VMEM((devices * qblocks, KEY_BLOCK, 2 * LANES), bf16),
            pltpu.VMEM((count, heads_width), bf16),
            pltpu.VMEM((count, heads_width), bf16),
            pltpu.VMEM((count, heads_width), bf16),
            pltpu.VMEM((out_weight.shape[0], half), bf16),
            pltpu.VMEM((count, half), f32),
            pltpu.VMEM((qblocks, 1, LANES), f32),
            pltpu.VMEM((qblocks, 1, LANES), f32),
            pltpu.SemaphoreType.DMA((devices,)),
            pltpu.SemaphoreType.DMA((devices,)),
            pltpu.SemaphoreType.DMA((2,)),
            pltpu.SemaphoreType.DMA((qblocks,)),
            pltpu.SemaphoreType.DMA((qblocks,)),
            pltpu.SemaphoreType.DMA((2,)),
        ],
        compiler_params=pltpu.CompilerParams(
            collective_id=0, has_side_effects=True, vmem_limit_bytes=60 * 1024 * 1024
        ),
    )(
        chosen_owner[0], chosen_part[0], row_data, query_weight, key_weight, value_weight,
        out_weight, norm_gain[None], cosine, sine,
    )
    return result[None]


def solution(mesh):
    placed = (
        P("dp", "kv", None),
        P(None, "tp"),
        P(None, "tp"),
        P(None, "tp"),
        P("tp", None),
        P("tp"),
        P("dp", None, None),
        P("dp", None, None),
    )
    return jax.shard_map(
        body, mesh=mesh, in_specs=placed, out_specs=P("dp", "kv", "tp"), check_vma=False
    )
```

```python
import functools

import jax
import jax.numpy as jnp
from jax import lax
from jax.experimental import pallas as pl
from jax.experimental.pallas import tpu as pltpu
from jax.sharding import PartitionSpec as P

HEAD_DIM = 64
QUERY_BLOCK = 128
KEY_BLOCK = 64
LANES = 128
ROWS = 256
COLS = 256

rope_base = 10000.0
norm_eps = 1e-06
MESH = pl.DeviceIdType.MESH


def turn(u, cosine, sine):
    lane = lax.broadcasted_iota(jnp.int32, u.shape, 1)
    half = HEAD_DIM // 2
    swapped = jnp.where(
        lane % HEAD_DIM < half, pltpu.roll(u, LANES - half, 1), pltpu.roll(u, half, 1)
    )
    return u * cosine + swapped * sine


def spread(pair, head):
    wide = pair.astype(jnp.float32)
    swapped = pltpu.roll(wide, HEAD_DIM, 1)
    low = lax.broadcasted_iota(jnp.int32, wide.shape, 1) < HEAD_DIM
    in_low, in_high = (wide, swapped) if head == 0 else (swapped, wide)
    return jnp.concatenate(
        [jnp.where(low, in_low, 0.0), jnp.where(low, 0.0, in_high)], axis=0
    ).astype(jnp.bfloat16)


def kernel(
    devices, ids_ref, tok, wq, wk, wv, ow, gain, cosine, sine, out,
    kv, send, pool, queries, mix, mix_other, ow_other, proj, ss, ss_other,
    kv_send, kv_recv, ow_sems, mix_send, mix_recv, ss_sems,
):
    me = lax.axis_index("kv")
    core = lax.axis_index("tp")
    other = 1 - core
    tokens = tok.shape[0]
    qblocks = tokens // QUERY_BLOCK
    chosen = ids_ref.shape[1]
    held = tokens // KEY_BLOCK
    half = ow_other.shape[1]
    row_steps = tokens // ROWS
    per_q = QUERY_BLOCK // KEY_BLOCK

    barrier = pltpu.get_barrier_semaphore()

    @pl.loop(0, devices)
    def _(j):
        @pl.when(j != me)
        def _():
            pl.semaphore_signal(barrier, inc=1, device_id={"kv": j}, device_id_type=MESH)

    pl.semaphore_signal(barrier, inc=1, device_id={"tp": other}, device_id_type=MESH)

    @pl.loop(0, row_steps)
    def _(r):
        rows = pl.ds(pl.multiple_of(r * ROWS, ROWS), ROWS)
        both = jnp.dot(
            tok[rows, :],
            jnp.concatenate([wk[...], wv[...]], axis=1),
            preferred_element_type=jnp.float32,
        )
        keys = turn(both[:, :LANES], cosine[rows, :], sine[rows, :])
        joined = jnp.concatenate([keys, both[:, LANES:]], axis=1).astype(jnp.bfloat16)
        blocks = ROWS // KEY_BLOCK
        kv[pl.ds(r * blocks, blocks)] = joined.reshape(blocks, KEY_BLOCK, 2 * LANES)

    pl.semaphore_wait(barrier, devices)

    def place(src, row, s):
        at = ids_ref[row, s] - src * held
        return jnp.logical_and(at >= 0, at < held), at

    def wanted(dst, q):
        found = [place(me, dst * qblocks + q, s) for s in range(chosen)]
        return sum(jnp.where(here, at, 0) for here, at in found)

    def kv_copy(src, dst, to, q):
        return pltpu.make_async_remote_copy(
            src_ref=send.at[pl.ds(q * devices + dst, 1)],
            dst_ref=pool.at[pl.ds(q * devices + src, 1)],
            send_sem=kv_send.at[q, dst],
            recv_sem=kv_recv.at[q, src],
            device_id={"kv": to},
            device_id_type=MESH,
        )

    @pl.loop(0, qblocks)
    def _(q):
        @pl.loop(0, devices)
        def _(dst):
            @pl.when(dst > me)
            def _():
                send[pl.ds(q * devices + dst, 1)] = kv[pl.ds(wanted(dst, q), 1)]
                kv_copy(me, dst, dst, q).start()

            @pl.when(dst == me)
            def _():
                pool[pl.ds(q * devices + me, 1)] = kv[pl.ds(wanted(me, q), 1)]

            @pl.when(dst > me)
            def _():
                pool[pl.ds(q * devices + dst, 1)] = jnp.zeros(
                    (1, KEY_BLOCK, 2 * LANES), jnp.bfloat16
                )

    ow_copy = pltpu.make_async_remote_copy(
        src_ref=ow.at[:, pl.ds(pl.multiple_of(other * half, half), half)],
        dst_ref=ow_other,
        send_sem=ow_sems.at[0],
        recv_sem=ow_sems.at[1],
        device_id={"tp": other},
        device_id_type=MESH,
    )
    ow_copy.start()

    @pl.loop(0, row_steps)
    def _(r):
        rows = pl.ds(pl.multiple_of(r * ROWS, ROWS), ROWS)
        for c in range(wq.shape[1] // COLS):
            part = jnp.dot(
                tok[rows, :], wq[:, c * COLS : (c + 1) * COLS], preferred_element_type=jnp.float32
            )
            for k in range(COLS // LANES):
                at = c * COLS + k * LANES
                queries[rows, at : at + LANES] = turn(
                    part[:, k * LANES : (k + 1) * LANES], cosine[rows, :], sine[rows, :]
                ).astype(jnp.bfloat16)

    kv_heads = wk.shape[1] // HEAD_DIM
    slices = wq.shape[1] // LANES // kv_heads
    key_count = devices * KEY_BLOCK + QUERY_BLOCK

    def mix_copy(b):
        rows = pl.ds(pl.multiple_of(b * QUERY_BLOCK, QUERY_BLOCK), QUERY_BLOCK)
        return pltpu.make_async_remote_copy(
            src_ref=mix.at[rows],
            dst_ref=mix_other.at[rows],
            send_sem=mix_send.at[b],
            recv_sem=mix_recv.at[b],
            device_id={"tp": other},
            device_id_type=MESH,
        )

    def attend(b):
        row = me * qblocks + b

        @pl.loop(0, devices)
        def _(src):
            @pl.when(src < me)
            def _():
                kv_copy(src, src, src, b).wait_recv()

        rows = pl.ds(pl.multiple_of(b * QUERY_BLOCK, QUERY_BLOCK), QUERY_BLOCK)
        pieces = [pool[pl.ds(b * devices, devices)].reshape(devices * KEY_BLOCK, 2 * LANES)]
        lane = lax.broadcasted_iota(jnp.int32, (1, devices * KEY_BLOCK), 1) // KEY_BLOCK
        far = jnp.full((1, devices * KEY_BLOCK), -jnp.inf, jnp.float32)
        for src in range(devices):
            named = sum(jnp.where(place(src, row, s)[0], 1, 0) for s in range(chosen))
            far = jnp.where(lane == src, jnp.where(named > 0, 0.0, -jnp.inf), far)
        pieces.append(kv[pl.ds(b * per_q, per_q)].reshape(QUERY_BLOCK, 2 * LANES))
        near = jnp.where(
            lax.broadcasted_iota(jnp.int32, (slices * QUERY_BLOCK, QUERY_BLOCK), 0) % QUERY_BLOCK
            >= lax.broadcasted_iota(jnp.int32, (slices * QUERY_BLOCK, QUERY_BLOCK), 1),
            0.0,
            -jnp.inf,
        )
        bias = jnp.concatenate(
            [jnp.broadcast_to(far, (slices * QUERY_BLOCK, devices * KEY_BLOCK)), near], axis=1
        )
        both = jnp.concatenate(pieces, axis=0)
        for n in range(kv_heads):
            q = jnp.concatenate(
                [
                    queries[rows, (n * slices + m) * LANES : (n * slices + m + 1) * LANES]
                    for m in range(slices)
                ],
                axis=0,
            )
            scores = lax.dot_general(
                q,
                spread(both[:, :LANES], n),
                (((1,), (1,)), ((), ())),
                preferred_element_type=jnp.float32,
            )
            probs = []
            for side in range(2):
                s = scores[:, side * key_count : (side + 1) * key_count] * HEAD_DIM**-0.5 + bias
                e = jnp.exp(s - jnp.max(s, axis=1, keepdims=True))
                probs.append((e * (1.0 / jnp.sum(e, axis=1, keepdims=True))).astype(jnp.bfloat16))
            mixed = jnp.dot(
                jnp.concatenate(probs, axis=1),
                spread(both[:, LANES:], n),
                preferred_element_type=jnp.float32,
            ).astype(jnp.bfloat16)
            for m in range(slices):
                at = (n * slices + m) * LANES
                mix[rows, at : at + LANES] = mixed[m * QUERY_BLOCK : (m + 1) * QUERY_BLOCK]
        mix_copy(b).start()

    blocks_in = ROWS // QUERY_BLOCK

    def project(r):
        for k in range(blocks_in):
            mix_copy(r * blocks_in + k).wait_recv()
        rows = pl.ds(pl.multiple_of(r * ROWS, ROWS), ROWS)
        total = jnp.zeros((ROWS, LANES), jnp.float32)
        for c in range(half // COLS):
            mine = jnp.dot(
                mix[rows, :],
                ow[:, pl.ds(pl.multiple_of(core * half + c * COLS, COLS), COLS)],
                preferred_element_type=jnp.float32,
            ).astype(jnp.bfloat16)
            theirs = jnp.dot(
                mix_other[rows, :],
                ow_other[:, c * COLS : (c + 1) * COLS],
                preferred_element_type=jnp.float32,
            ).astype(jnp.bfloat16)
            added = mine.astype(jnp.float32) + theirs.astype(jnp.float32)
            proj[rows, c * COLS : (c + 1) * COLS] = added
            for k in range(COLS // LANES):
                piece = added[:, k * LANES : (k + 1) * LANES]
                total = total + piece * piece
        for k in range(ROWS // LANES):
            ss[r * (ROWS // LANES) + k] = jnp.sum(
                total[k * LANES : (k + 1) * LANES].T, axis=0, keepdims=True
            )

    ow_copy.wait_recv()

    @pl.loop(0, row_steps)
    def _(r):
        @pl.loop(0, blocks_in)
        def _(k):
            attend(r * blocks_in + k)

        @pl.when(r > 0)
        def _():
            project(r - 1)

    project(row_steps - 1)

    ss_copy = pltpu.make_async_remote_copy(
        src_ref=ss,
        dst_ref=ss_other,
        send_sem=ss_sems.at[0],
        recv_sem=ss_sems.at[1],
        device_id={"tp": other},
        device_id_type=MESH,
    )
    ss_copy.start()

    @pl.loop(0, qblocks)
    def _(q):
        @pl.loop(0, devices)
        def _(dst):
            @pl.when(dst > me)
            def _():
                kv_copy(me, dst, dst, q).wait_send()

    ow_copy.wait_send()

    @pl.loop(0, qblocks)
    def _(b):
        mix_copy(b).wait_send()

    ss_copy.wait()

    @pl.loop(0, qblocks)
    def _(b):
        rows = pl.ds(pl.multiple_of(b * LANES, LANES), LANES)
        scale = lax.rsqrt((ss[b] + ss_other[b]) / (2 * half) + norm_eps)
        scale = jnp.broadcast_to(scale, (LANES, LANES)).T
        for c in range(half // LANES):
            at = slice(c * LANES, (c + 1) * LANES)
            out[rows, at] = (proj[rows, at] * scale * gain[:, at]).astype(jnp.bfloat16)


def body(
    tokens, query_weight, key_weight, value_weight, out_weight, norm_gain, chosen_owner, chosen_part
):
    row_data = tokens[0]
    count = row_data.shape[0]
    devices = lax.axis_size("kv")
    qblocks = count // QUERY_BLOCK
    positions = lax.axis_index("kv") * count + jnp.arange(count, dtype=jnp.int32)
    half_dim = HEAD_DIM // 2
    lane = jnp.arange(LANES, dtype=jnp.int32)
    frequency = rope_base ** (-(lane % half_dim).astype(jnp.float32) / half_dim)
    angles = positions.astype(jnp.float32)[:, None] * frequency
    cosine = jnp.cos(angles)
    sine = jnp.where(lane % HEAD_DIM < half_dim, -1.0, 1.0) * jnp.sin(angles)
    ids = jnp.where(
        chosen_owner[0] >= 0, chosen_owner[0] * (count // KEY_BLOCK) + chosen_part[0], -1
    )
    heads_width = query_weight.shape[1]
    half = norm_gain.shape[0]
    vmem = pl.BlockSpec(memory_space=pltpu.VMEM)
    smem = pl.BlockSpec(memory_space=pltpu.SMEM)
    bf16, f32 = jnp.bfloat16, jnp.float32
    result = pl.pallas_call(
        functools.partial(kernel, devices),
        out_shape=jax.ShapeDtypeStruct((count, half), bf16),
        in_specs=[smem] + [vmem] * 8,
        out_specs=vmem,
        scratch_shapes=[
            pltpu.VMEM((count // KEY_BLOCK, KEY_BLOCK, 2 * LANES), bf16),
            pltpu.VMEM((devices * qblocks, KEY_BLOCK, 2 * LANES), bf16),
            pltpu.VMEM((devices * qblocks, KEY_BLOCK, 2 * LANES), bf16),
            pltpu.VMEM((count, heads_width), bf16),
            pltpu.VMEM((count, heads_width), bf16),
            pltpu.VMEM((count, heads_width), bf16),
            pltpu.VMEM((out_weight.shape[0], half), bf16),
            pltpu.VMEM((count, half), f32),
            pltpu.VMEM((qblocks, 1, LANES), f32),
            pltpu.VMEM((qblocks, 1, LANES), f32),
            pltpu.SemaphoreType.DMA((qblocks, devices)),
            pltpu.SemaphoreType.DMA((qblocks, devices)),
            pltpu.SemaphoreType.DMA((2,)),
            pltpu.SemaphoreType.DMA((qblocks,)),
            pltpu.SemaphoreType.DMA((qblocks,)),
            pltpu.SemaphoreType.DMA((2,)),
        ],
        compiler_params=pltpu.CompilerParams(
            collective_id=0, has_side_effects=True, vmem_limit_bytes=60 * 1024 * 1024
        ),
    )(
        ids, row_data, query_weight, key_weight, value_weight,
        out_weight, norm_gain[None], cosine, sine,
    )
    return result[None]


def solution(mesh):
    placed = (
        P("dp", "kv", None),
        P(None, "tp"),
        P(None, "tp"),
        P(None, "tp"),
        P("tp", None),
        P("tp"),
        P("dp", None, None),
        P("dp", None, None),
    )
    return jax.shard_map(
        body, mesh=mesh, in_specs=placed, out_specs=P("dp", "kv", "tp"), check_vma=False
    )
```

```python
import functools

import jax
import jax.numpy as jnp
from jax import lax
from jax.experimental import pallas as pl
from jax.experimental.pallas import tpu as pltpu
from jax.sharding import PartitionSpec as P

HEAD_DIM = 64
QUERY_BLOCK = 128
KEY_BLOCK = 64
LANES = 128
ROWS = 256
COLS = 256

rope_base = 10000.0
norm_eps = 1e-06
MESH = pl.DeviceIdType.MESH


def turn(u, cosine, sine):
    lane = lax.broadcasted_iota(jnp.int32, u.shape, 1)
    half = HEAD_DIM // 2
    swapped = jnp.where(
        lane % HEAD_DIM < half, pltpu.roll(u, LANES - half, 1), pltpu.roll(u, half, 1)
    )
    return u * cosine + swapped * sine


def spread(pair, head):
    wide = pair.astype(jnp.float32)
    swapped = pltpu.roll(wide, HEAD_DIM, 1)
    low = lax.broadcasted_iota(jnp.int32, wide.shape, 1) < HEAD_DIM
    in_low, in_high = (wide, swapped) if head == 0 else (swapped, wide)
    return jnp.concatenate(
        [jnp.where(low, in_low, 0.0), jnp.where(low, 0.0, in_high)], axis=0
    ).astype(jnp.bfloat16)


def kernel(
    devices, ids_ref, tok_hbm, wq_hbm, wk_hbm, wv_hbm, ow_hbm, gain, cosine, sine, out,
    tok, wq, wkv, ow, tok_sems, weight_sems,
    kv, send, pool, queries, mix, mix_other, ow_other, proj, ss, ss_other,
    kv_send, kv_recv, ow_sems, mix_send, mix_recv, ss_sems,
):
    me = lax.axis_index("kv")
    core = lax.axis_index("tp")
    other = 1 - core
    tokens = tok.shape[0]
    qblocks = tokens // QUERY_BLOCK
    chosen = ids_ref.shape[1]
    held = tokens // KEY_BLOCK
    half = ow_other.shape[1]
    row_steps = tokens // ROWS
    per_q = QUERY_BLOCK // KEY_BLOCK

    key_width = wk_hbm.shape[1]

    def tok_copy(r):
        rows = pl.ds(pl.multiple_of(r * ROWS, ROWS), ROWS)
        return pltpu.make_async_copy(tok_hbm.at[rows], tok.at[rows], tok_sems.at[r])

    wk_copy = pltpu.make_async_copy(wk_hbm, wkv.at[:, pl.ds(0, key_width)], weight_sems.at[0])
    wv_copy = pltpu.make_async_copy(
        wv_hbm, wkv.at[:, pl.ds(key_width, key_width)], weight_sems.at[1]
    )
    wq_copy = pltpu.make_async_copy(wq_hbm, wq, weight_sems.at[2])
    ow_load = pltpu.make_async_copy(ow_hbm, ow, weight_sems.at[3])
    wk_copy.start()
    wv_copy.start()
    for r in range(row_steps):
        tok_copy(r).start()
    wq_copy.start()
    ow_load.start()

    barrier = pltpu.get_barrier_semaphore()

    @pl.loop(0, devices)
    def _(j):
        @pl.when(j != me)
        def _():
            pl.semaphore_signal(barrier, inc=1, device_id={"kv": j}, device_id_type=MESH)

    pl.semaphore_signal(barrier, inc=1, device_id={"tp": other}, device_id_type=MESH)

    wk_copy.wait()
    wv_copy.wait()

    @pl.loop(0, row_steps)
    def _(r):
        tok_copy(r).wait()
        rows = pl.ds(pl.multiple_of(r * ROWS, ROWS), ROWS)
        both = jnp.dot(
            tok[rows, :],
            wkv[...],
            preferred_element_type=jnp.float32,
        )
        keys = turn(both[:, :LANES], cosine[rows, :], sine[rows, :])
        joined = jnp.concatenate([keys, both[:, LANES:]], axis=1).astype(jnp.bfloat16)
        blocks = ROWS // KEY_BLOCK
        kv[pl.ds(r * blocks, blocks)] = joined.reshape(blocks, KEY_BLOCK, 2 * LANES)

    pl.semaphore_wait(barrier, devices)

    def place(src, row, s):
        at = ids_ref[row, s] - src * held
        return jnp.logical_and(at >= 0, at < held), at

    def wanted(dst, q):
        found = [place(me, dst * qblocks + q, s) for s in range(chosen)]
        return sum(jnp.where(here, at, 0) for here, at in found)

    def kv_copy(src, dst, to, q):
        return pltpu.make_async_remote_copy(
            src_ref=send.at[pl.ds(q * devices + dst, 1)],
            dst_ref=pool.at[pl.ds(q * devices + src, 1)],
            send_sem=kv_send.at[q, dst],
            recv_sem=kv_recv.at[q, src],
            device_id={"kv": to},
            device_id_type=MESH,
        )

    @pl.loop(0, qblocks)
    def _(q):
        @pl.loop(0, devices)
        def _(dst):
            @pl.when(dst > me)
            def _():
                send[pl.ds(q * devices + dst, 1)] = kv[pl.ds(wanted(dst, q), 1)]
                kv_copy(me, dst, dst, q).start()

            @pl.when(dst == me)
            def _():
                pool[pl.ds(q * devices + me, 1)] = kv[pl.ds(wanted(me, q), 1)]

            @pl.when(dst > me)
            def _():
                pool[pl.ds(q * devices + dst, 1)] = jnp.zeros(
                    (1, KEY_BLOCK, 2 * LANES), jnp.bfloat16
                )

    ow_copy = pltpu.make_async_remote_copy(
        src_ref=ow.at[:, pl.ds(pl.multiple_of(other * half, half), half)],
        dst_ref=ow_other,
        send_sem=ow_sems.at[0],
        recv_sem=ow_sems.at[1],
        device_id={"tp": other},
        device_id_type=MESH,
    )
    ow_load.wait()
    ow_copy.start()
    wq_copy.wait()

    @pl.loop(0, row_steps)
    def _(r):
        rows = pl.ds(pl.multiple_of(r * ROWS, ROWS), ROWS)
        for c in range(wq.shape[1] // COLS):
            part = jnp.dot(
                tok[rows, :], wq[:, c * COLS : (c + 1) * COLS], preferred_element_type=jnp.float32
            )
            for k in range(COLS // LANES):
                at = c * COLS + k * LANES
                queries[rows, at : at + LANES] = turn(
                    part[:, k * LANES : (k + 1) * LANES], cosine[rows, :], sine[rows, :]
                ).astype(jnp.bfloat16)

    kv_heads = key_width // HEAD_DIM
    slices = wq.shape[1] // LANES // kv_heads
    key_count = devices * KEY_BLOCK + QUERY_BLOCK

    def mix_copy(b):
        rows = pl.ds(pl.multiple_of(b * QUERY_BLOCK, QUERY_BLOCK), QUERY_BLOCK)
        return pltpu.make_async_remote_copy(
            src_ref=mix.at[rows],
            dst_ref=mix_other.at[rows],
            send_sem=mix_send.at[b],
            recv_sem=mix_recv.at[b],
            device_id={"tp": other},
            device_id_type=MESH,
        )

    def attend(b):
        row = me * qblocks + b

        @pl.loop(0, devices)
        def _(src):
            @pl.when(src < me)
            def _():
                kv_copy(src, src, src, b).wait_recv()

        rows = pl.ds(pl.multiple_of(b * QUERY_BLOCK, QUERY_BLOCK), QUERY_BLOCK)
        pieces = [pool[pl.ds(b * devices, devices)].reshape(devices * KEY_BLOCK, 2 * LANES)]
        lane = lax.broadcasted_iota(jnp.int32, (1, devices * KEY_BLOCK), 1) // KEY_BLOCK
        far = jnp.full((1, devices * KEY_BLOCK), -jnp.inf, jnp.float32)
        for src in range(devices):
            named = sum(jnp.where(place(src, row, s)[0], 1, 0) for s in range(chosen))
            far = jnp.where(lane == src, jnp.where(named > 0, 0.0, -jnp.inf), far)
        pieces.append(kv[pl.ds(b * per_q, per_q)].reshape(QUERY_BLOCK, 2 * LANES))
        near = jnp.where(
            lax.broadcasted_iota(jnp.int32, (slices * QUERY_BLOCK, QUERY_BLOCK), 0) % QUERY_BLOCK
            >= lax.broadcasted_iota(jnp.int32, (slices * QUERY_BLOCK, QUERY_BLOCK), 1),
            0.0,
            -jnp.inf,
        )
        bias = jnp.concatenate(
            [jnp.broadcast_to(far, (slices * QUERY_BLOCK, devices * KEY_BLOCK)), near], axis=1
        )
        both = jnp.concatenate(pieces, axis=0)
        for n in range(kv_heads):
            q = jnp.concatenate(
                [
                    queries[rows, (n * slices + m) * LANES : (n * slices + m + 1) * LANES]
                    for m in range(slices)
                ],
                axis=0,
            )
            scores = lax.dot_general(
                q,
                spread(both[:, :LANES], n),
                (((1,), (1,)), ((), ())),
                preferred_element_type=jnp.float32,
            )
            probs = []
            for side in range(2):
                s = scores[:, side * key_count : (side + 1) * key_count] * HEAD_DIM**-0.5 + bias
                e = jnp.exp(s - jnp.max(s, axis=1, keepdims=True))
                probs.append((e * (1.0 / jnp.sum(e, axis=1, keepdims=True))).astype(jnp.bfloat16))
            mixed = jnp.dot(
                jnp.concatenate(probs, axis=1),
                spread(both[:, LANES:], n),
                preferred_element_type=jnp.float32,
            ).astype(jnp.bfloat16)
            for m in range(slices):
                at = (n * slices + m) * LANES
                mix[rows, at : at + LANES] = mixed[m * QUERY_BLOCK : (m + 1) * QUERY_BLOCK]
        mix_copy(b).start()

    blocks_in = ROWS // QUERY_BLOCK

    def project(r):
        for k in range(blocks_in):
            mix_copy(r * blocks_in + k).wait_recv()
        rows = pl.ds(pl.multiple_of(r * ROWS, ROWS), ROWS)
        total = jnp.zeros((ROWS, LANES), jnp.float32)
        for c in range(half // COLS):
            mine = jnp.dot(
                mix[rows, :],
                ow[:, pl.ds(pl.multiple_of(core * half + c * COLS, COLS), COLS)],
                preferred_element_type=jnp.float32,
            ).astype(jnp.bfloat16)
            theirs = jnp.dot(
                mix_other[rows, :],
                ow_other[:, c * COLS : (c + 1) * COLS],
                preferred_element_type=jnp.float32,
            ).astype(jnp.bfloat16)
            added = mine.astype(jnp.float32) + theirs.astype(jnp.float32)
            proj[rows, c * COLS : (c + 1) * COLS] = added
            for k in range(COLS // LANES):
                piece = added[:, k * LANES : (k + 1) * LANES]
                total = total + piece * piece
        for k in range(ROWS // LANES):
            ss[r * (ROWS // LANES) + k] = jnp.sum(
                total[k * LANES : (k + 1) * LANES].T, axis=0, keepdims=True
            )

    ow_copy.wait_recv()

    @pl.loop(0, row_steps)
    def _(r):
        @pl.loop(0, blocks_in)
        def _(k):
            attend(r * blocks_in + k)

        @pl.when(r > 0)
        def _():
            project(r - 1)

    project(row_steps - 1)

    ss_copy = pltpu.make_async_remote_copy(
        src_ref=ss,
        dst_ref=ss_other,
        send_sem=ss_sems.at[0],
        recv_sem=ss_sems.at[1],
        device_id={"tp": other},
        device_id_type=MESH,
    )
    ss_copy.start()

    @pl.loop(0, qblocks)
    def _(q):
        @pl.loop(0, devices)
        def _(dst):
            @pl.when(dst > me)
            def _():
                kv_copy(me, dst, dst, q).wait_send()

    ow_copy.wait_send()

    @pl.loop(0, qblocks)
    def _(b):
        mix_copy(b).wait_send()

    ss_copy.wait()

    @pl.loop(0, qblocks)
    def _(b):
        rows = pl.ds(pl.multiple_of(b * LANES, LANES), LANES)
        scale = lax.rsqrt((ss[b] + ss_other[b]) / (2 * half) + norm_eps)
        scale = jnp.broadcast_to(scale, (LANES, LANES)).T
        for c in range(half // LANES):
            at = slice(c * LANES, (c + 1) * LANES)
            out[rows, at] = (proj[rows, at] * scale * gain[:, at]).astype(jnp.bfloat16)


def body(
    tokens, query_weight, key_weight, value_weight, out_weight, norm_gain, chosen_owner, chosen_part
):
    row_data = tokens[0]
    count = row_data.shape[0]
    devices = lax.axis_size("kv")
    qblocks = count // QUERY_BLOCK
    positions = lax.axis_index("kv") * count + jnp.arange(count, dtype=jnp.int32)
    half_dim = HEAD_DIM // 2
    lane = jnp.arange(LANES, dtype=jnp.int32)
    frequency = rope_base ** (-(lane % half_dim).astype(jnp.float32) / half_dim)
    angles = positions.astype(jnp.float32)[:, None] * frequency
    cosine = jnp.cos(angles)
    sine = jnp.where(lane % HEAD_DIM < half_dim, -1.0, 1.0) * jnp.sin(angles)
    ids = jnp.where(
        chosen_owner[0] >= 0, chosen_owner[0] * (count // KEY_BLOCK) + chosen_part[0], -1
    )
    heads_width = query_weight.shape[1]
    half = norm_gain.shape[0]
    vmem = pl.BlockSpec(memory_space=pltpu.VMEM)
    smem = pl.BlockSpec(memory_space=pltpu.SMEM)
    bf16, f32 = jnp.bfloat16, jnp.float32
    result = pl.pallas_call(
        functools.partial(kernel, devices),
        out_shape=jax.ShapeDtypeStruct((count, half), bf16),
        in_specs=[smem] + [pl.BlockSpec(memory_space=pl.ANY)] * 5 + [vmem] * 3,
        out_specs=vmem,
        scratch_shapes=[
            pltpu.VMEM(row_data.shape, bf16),
            pltpu.VMEM(query_weight.shape, bf16),
            pltpu.VMEM((key_weight.shape[0], 2 * key_weight.shape[1]), bf16),
            pltpu.VMEM(out_weight.shape, bf16),
            pltpu.SemaphoreType.DMA((count // ROWS,)),
            pltpu.SemaphoreType.DMA((4,)),
            pltpu.VMEM((count // KEY_BLOCK, KEY_BLOCK, 2 * LANES), bf16),
            pltpu.VMEM((devices * qblocks, KEY_BLOCK, 2 * LANES), bf16),
            pltpu.VMEM((devices * qblocks, KEY_BLOCK, 2 * LANES), bf16),
            pltpu.VMEM((count, heads_width), bf16),
            pltpu.VMEM((count, heads_width), bf16),
            pltpu.VMEM((count, heads_width), bf16),
            pltpu.VMEM((out_weight.shape[0], half), bf16),
            pltpu.VMEM((count, half), f32),
            pltpu.VMEM((qblocks, 1, LANES), f32),
            pltpu.VMEM((qblocks, 1, LANES), f32),
            pltpu.SemaphoreType.DMA((qblocks, devices)),
            pltpu.SemaphoreType.DMA((qblocks, devices)),
            pltpu.SemaphoreType.DMA((2,)),
            pltpu.SemaphoreType.DMA((qblocks,)),
            pltpu.SemaphoreType.DMA((qblocks,)),
            pltpu.SemaphoreType.DMA((2,)),
        ],
        compiler_params=pltpu.CompilerParams(
            collective_id=0, has_side_effects=True, vmem_limit_bytes=60 * 1024 * 1024
        ),
    )(
        ids, row_data, query_weight, key_weight, value_weight,
        out_weight, norm_gain[None], cosine, sine,
    )
    return result[None]


def solution(mesh):
    placed = (
        P("dp", "kv", None),
        P(None, "tp"),
        P(None, "tp"),
        P(None, "tp"),
        P("tp", None),
        P("tp"),
        P("dp", None, None),
        P("dp", None, None),
    )
    return jax.shard_map(
        body, mesh=mesh, in_specs=placed, out_specs=P("dp", "kv", "tp"), check_vma=False
    )
```

```python
import functools

import jax
import jax.numpy as jnp
import numpy as np
from jax import lax
from jax.experimental import pallas as pl
from jax.experimental.pallas import tpu as pltpu
from jax.sharding import PartitionSpec as P

HEAD_DIM = 64
QUERY_BLOCK = 128
KEY_BLOCK = 64
LANES = 128
ROWS = 256
COLS = 256

rope_base = 10000.0
norm_eps = 1e-06
MESH = pl.DeviceIdType.MESH


def turn(u, cosine, sine):
    lane = lax.broadcasted_iota(jnp.int32, u.shape, 1)
    half = HEAD_DIM // 2
    swapped = jnp.where(
        lane % HEAD_DIM < half, pltpu.roll(u, LANES - half, 1), pltpu.roll(u, half, 1)
    )
    return u * cosine + swapped * sine


def spread(pair, head):
    wide = pair.astype(jnp.float32)
    swapped = pltpu.roll(wide, HEAD_DIM, 1)
    low = lax.broadcasted_iota(jnp.int32, wide.shape, 1) < HEAD_DIM
    in_low, in_high = (wide, swapped) if head == 0 else (swapped, wide)
    return jnp.concatenate(
        [jnp.where(low, in_low, 0.0), jnp.where(low, 0.0, in_high)], axis=0
    ).astype(jnp.bfloat16)


def kernel(
    devices, ids_ref, tok_hbm, wq_hbm, wk_hbm, wv_hbm, ow_hbm, gain, far_cos, far_sin, near_cos, near_sin, out,
    cosine, sine,
    tok, wq, wkv, ow, tok_sems, weight_sems,
    kv, send, pool, queries, mix, mix_other, ow_other, proj, ss, ss_other,
    kv_send, kv_recv, ow_sems, mix_send, mix_recv, ss_sems,
):
    me = lax.axis_index("kv")
    core = lax.axis_index("tp")
    other = 1 - core
    tokens = tok.shape[0]
    qblocks = tokens // QUERY_BLOCK
    chosen = ids_ref.shape[1]
    held = tokens // KEY_BLOCK
    half = ow_other.shape[1]
    row_steps = tokens // ROWS
    per_q = QUERY_BLOCK // KEY_BLOCK

    key_width = wk_hbm.shape[1]

    def tok_copy(r):
        rows = pl.ds(pl.multiple_of(r * ROWS, ROWS), ROWS)
        return pltpu.make_async_copy(tok_hbm.at[rows], tok.at[rows], tok_sems.at[r])

    wk_copy = pltpu.make_async_copy(wk_hbm, wkv.at[:, pl.ds(0, key_width)], weight_sems.at[0])
    wv_copy = pltpu.make_async_copy(
        wv_hbm, wkv.at[:, pl.ds(key_width, key_width)], weight_sems.at[1]
    )
    wq_copy = pltpu.make_async_copy(wq_hbm, wq, weight_sems.at[2])
    ow_load = pltpu.make_async_copy(ow_hbm, ow, weight_sems.at[3])
    wk_copy.start()
    wv_copy.start()
    for r in range(row_steps):
        tok_copy(r).start()
    wq_copy.start()
    ow_load.start()

    barrier = pltpu.get_barrier_semaphore()

    @pl.loop(0, devices)
    def _(j):
        @pl.when(j != me)
        def _():
            pl.semaphore_signal(barrier, inc=1, device_id={"kv": j}, device_id_type=MESH)

    pl.semaphore_signal(barrier, inc=1, device_id={"tp": other}, device_id_type=MESH)

    @pl.loop(0, qblocks)
    def _(b):
        rows = pl.ds(pl.multiple_of(b * QUERY_BLOCK, QUERY_BLOCK), QUERY_BLOCK)
        cosine[rows, :] = far_cos[b] * near_cos[...] - far_sin[b] * near_sin[...]
        sine[rows, :] = far_sin[b] * near_cos[...] + far_cos[b] * near_sin[...]

    wk_copy.wait()
    wv_copy.wait()

    @pl.loop(0, row_steps)
    def _(r):
        tok_copy(r).wait()
        rows = pl.ds(pl.multiple_of(r * ROWS, ROWS), ROWS)
        both = jnp.dot(
            tok[rows, :],
            wkv[...],
            preferred_element_type=jnp.float32,
        )
        keys = turn(both[:, :LANES], cosine[rows, :], sine[rows, :])
        joined = jnp.concatenate([keys, both[:, LANES:]], axis=1).astype(jnp.bfloat16)
        blocks = ROWS // KEY_BLOCK
        kv[pl.ds(r * blocks, blocks)] = joined.reshape(blocks, KEY_BLOCK, 2 * LANES)

    pl.semaphore_wait(barrier, devices)

    def place(src, row, s):
        at = ids_ref[row, s] - src * held
        return jnp.logical_and(at >= 0, at < held), at

    def wanted(dst, q):
        found = [place(me, dst * qblocks + q, s) for s in range(chosen)]
        return sum(jnp.where(here, at, 0) for here, at in found)

    def kv_copy(src, dst, to, q):
        return pltpu.make_async_remote_copy(
            src_ref=send.at[pl.ds(q * devices + dst, 1)],
            dst_ref=pool.at[pl.ds(q * devices + src, 1)],
            send_sem=kv_send.at[q, dst],
            recv_sem=kv_recv.at[q, src],
            device_id={"kv": to},
            device_id_type=MESH,
        )

    @pl.loop(0, qblocks)
    def _(q):
        @pl.loop(0, devices)
        def _(dst):
            @pl.when(dst > me)
            def _():
                send[pl.ds(q * devices + dst, 1)] = kv[pl.ds(wanted(dst, q), 1)]
                kv_copy(me, dst, dst, q).start()

            @pl.when(dst == me)
            def _():
                pool[pl.ds(q * devices + me, 1)] = kv[pl.ds(wanted(me, q), 1)]

            @pl.when(dst > me)
            def _():
                pool[pl.ds(q * devices + dst, 1)] = jnp.zeros(
                    (1, KEY_BLOCK, 2 * LANES), jnp.bfloat16
                )

    ow_copy = pltpu.make_async_remote_copy(
        src_ref=ow.at[:, pl.ds(pl.multiple_of(other * half, half), half)],
        dst_ref=ow_other,
        send_sem=ow_sems.at[0],
        recv_sem=ow_sems.at[1],
        device_id={"tp": other},
        device_id_type=MESH,
    )
    ow_load.wait()
    ow_copy.start()
    wq_copy.wait()

    @pl.loop(0, row_steps)
    def _(r):
        rows = pl.ds(pl.multiple_of(r * ROWS, ROWS), ROWS)
        for c in range(wq.shape[1] // COLS):
            part = jnp.dot(
                tok[rows, :], wq[:, c * COLS : (c + 1) * COLS], preferred_element_type=jnp.float32
            )
            for k in range(COLS // LANES):
                at = c * COLS + k * LANES
                queries[rows, at : at + LANES] = turn(
                    part[:, k * LANES : (k + 1) * LANES], cosine[rows, :], sine[rows, :]
                ).astype(jnp.bfloat16)

    kv_heads = key_width // HEAD_DIM
    slices = wq.shape[1] // LANES // kv_heads
    key_count = devices * KEY_BLOCK + QUERY_BLOCK

    def mix_copy(b):
        rows = pl.ds(pl.multiple_of(b * QUERY_BLOCK, QUERY_BLOCK), QUERY_BLOCK)
        return pltpu.make_async_remote_copy(
            src_ref=mix.at[rows],
            dst_ref=mix_other.at[rows],
            send_sem=mix_send.at[b],
            recv_sem=mix_recv.at[b],
            device_id={"tp": other},
            device_id_type=MESH,
        )

    def attend(b):
        row = me * qblocks + b

        @pl.loop(0, devices)
        def _(src):
            @pl.when(src < me)
            def _():
                kv_copy(src, src, src, b).wait_recv()

        rows = pl.ds(pl.multiple_of(b * QUERY_BLOCK, QUERY_BLOCK), QUERY_BLOCK)
        pieces = [pool[pl.ds(b * devices, devices)].reshape(devices * KEY_BLOCK, 2 * LANES)]
        lane = lax.broadcasted_iota(jnp.int32, (1, devices * KEY_BLOCK), 1) // KEY_BLOCK
        far = jnp.full((1, devices * KEY_BLOCK), -jnp.inf, jnp.float32)
        for src in range(devices):
            named = sum(jnp.where(place(src, row, s)[0], 1, 0) for s in range(chosen))
            far = jnp.where(lane == src, jnp.where(named > 0, 0.0, -jnp.inf), far)
        pieces.append(kv[pl.ds(b * per_q, per_q)].reshape(QUERY_BLOCK, 2 * LANES))
        near = jnp.where(
            lax.broadcasted_iota(jnp.int32, (slices * QUERY_BLOCK, QUERY_BLOCK), 0) % QUERY_BLOCK
            >= lax.broadcasted_iota(jnp.int32, (slices * QUERY_BLOCK, QUERY_BLOCK), 1),
            0.0,
            -jnp.inf,
        )
        bias = jnp.concatenate(
            [jnp.broadcast_to(far, (slices * QUERY_BLOCK, devices * KEY_BLOCK)), near], axis=1
        )
        both = jnp.concatenate(pieces, axis=0)
        for n in range(kv_heads):
            q = jnp.concatenate(
                [
                    queries[rows, (n * slices + m) * LANES : (n * slices + m + 1) * LANES]
                    for m in range(slices)
                ],
                axis=0,
            )
            scores = lax.dot_general(
                q,
                spread(both[:, :LANES], n),
                (((1,), (1,)), ((), ())),
                preferred_element_type=jnp.float32,
            )
            probs = []
            for side in range(2):
                s = scores[:, side * key_count : (side + 1) * key_count] * HEAD_DIM**-0.5 + bias
                e = jnp.exp(s - jnp.max(s, axis=1, keepdims=True))
                probs.append((e * (1.0 / jnp.sum(e, axis=1, keepdims=True))).astype(jnp.bfloat16))
            mixed = jnp.dot(
                jnp.concatenate(probs, axis=1),
                spread(both[:, LANES:], n),
                preferred_element_type=jnp.float32,
            ).astype(jnp.bfloat16)
            for m in range(slices):
                at = (n * slices + m) * LANES
                mix[rows, at : at + LANES] = mixed[m * QUERY_BLOCK : (m + 1) * QUERY_BLOCK]
        mix_copy(b).start()

    blocks_in = ROWS // QUERY_BLOCK

    def project(r):
        for k in range(blocks_in):
            mix_copy(r * blocks_in + k).wait_recv()
        rows = pl.ds(pl.multiple_of(r * ROWS, ROWS), ROWS)
        total = jnp.zeros((ROWS, LANES), jnp.float32)
        for c in range(half // COLS):
            mine = jnp.dot(
                mix[rows, :],
                ow[:, pl.ds(pl.multiple_of(core * half + c * COLS, COLS), COLS)],
                preferred_element_type=jnp.float32,
            ).astype(jnp.bfloat16)
            theirs = jnp.dot(
                mix_other[rows, :],
                ow_other[:, c * COLS : (c + 1) * COLS],
                preferred_element_type=jnp.float32,
            ).astype(jnp.bfloat16)
            added = mine.astype(jnp.float32) + theirs.astype(jnp.float32)
            proj[rows, c * COLS : (c + 1) * COLS] = added
            for k in range(COLS // LANES):
                piece = added[:, k * LANES : (k + 1) * LANES]
                total = total + piece * piece
        for k in range(ROWS // LANES):
            ss[r * (ROWS // LANES) + k] = jnp.sum(
                total[k * LANES : (k + 1) * LANES].T, axis=0, keepdims=True
            )

    ow_copy.wait_recv()

    @pl.loop(0, row_steps)
    def _(r):
        @pl.loop(0, blocks_in)
        def _(k):
            attend(r * blocks_in + k)

        @pl.when(r > 0)
        def _():
            project(r - 1)

    project(row_steps - 1)

    ss_copy = pltpu.make_async_remote_copy(
        src_ref=ss,
        dst_ref=ss_other,
        send_sem=ss_sems.at[0],
        recv_sem=ss_sems.at[1],
        device_id={"tp": other},
        device_id_type=MESH,
    )
    ss_copy.start()

    @pl.loop(0, qblocks)
    def _(q):
        @pl.loop(0, devices)
        def _(dst):
            @pl.when(dst > me)
            def _():
                kv_copy(me, dst, dst, q).wait_send()

    ow_copy.wait_send()

    @pl.loop(0, qblocks)
    def _(b):
        mix_copy(b).wait_send()

    ss_copy.wait()

    @pl.loop(0, qblocks)
    def _(b):
        rows = pl.ds(pl.multiple_of(b * LANES, LANES), LANES)
        scale = lax.rsqrt((ss[b] + ss_other[b]) / (2 * half) + norm_eps)
        scale = jnp.broadcast_to(scale, (LANES, LANES)).T
        for c in range(half // LANES):
            at = slice(c * LANES, (c + 1) * LANES)
            out[rows, at] = (proj[rows, at] * scale * gain[:, at]).astype(jnp.bfloat16)


def body(
    tokens, query_weight, key_weight, value_weight, out_weight, norm_gain, chosen_owner, chosen_part
):
    row_data = tokens[0]
    count = row_data.shape[0]
    devices = lax.axis_size("kv")
    qblocks = count // QUERY_BLOCK
    half_dim = HEAD_DIM // 2
    lane = np.arange(LANES)
    frequency = (rope_base ** (-(lane % half_dim) / half_dim)).astype(np.float32)
    sign = np.where(lane % HEAD_DIM < half_dim, -1.0, 1.0).astype(np.float32)
    inner = np.arange(QUERY_BLOCK)[:, None] * frequency.astype(np.float64)
    near_cos = np.cos(inner).astype(np.float32)
    near_sin = (sign * np.sin(inner)).astype(np.float32)
    starts = lax.axis_index("kv") * count + QUERY_BLOCK * jnp.arange(qblocks, dtype=jnp.int32)
    angles = starts.astype(jnp.float32)[:, None, None] * frequency
    far_cos, far_sin = jnp.cos(angles), sign * jnp.sin(angles)
    ids = jnp.where(
        chosen_owner[0] >= 0, chosen_owner[0] * (count // KEY_BLOCK) + chosen_part[0], -1
    )
    heads_width = query_weight.shape[1]
    half = norm_gain.shape[0]
    vmem = pl.BlockSpec(memory_space=pltpu.VMEM)
    smem = pl.BlockSpec(memory_space=pltpu.SMEM)
    bf16, f32 = jnp.bfloat16, jnp.float32
    result = pl.pallas_call(
        functools.partial(kernel, devices),
        out_shape=jax.ShapeDtypeStruct((count, half), bf16),
        in_specs=[smem] + [pl.BlockSpec(memory_space=pl.ANY)] * 5 + [vmem] * 5,
        out_specs=vmem,
        scratch_shapes=[
            pltpu.VMEM((count, LANES), f32),
            pltpu.VMEM((count, LANES), f32),
            pltpu.VMEM(row_data.shape, bf16),
            pltpu.VMEM(query_weight.shape, bf16),
            pltpu.VMEM((key_weight.shape[0], 2 * key_weight.shape[1]), bf16),
            pltpu.VMEM(out_weight.shape, bf16),
            pltpu.SemaphoreType.DMA((count // ROWS,)),
            pltpu.SemaphoreType.DMA((4,)),
            pltpu.VMEM((count // KEY_BLOCK, KEY_BLOCK, 2 * LANES), bf16),
            pltpu.VMEM((devices * qblocks, KEY_BLOCK, 2 * LANES), bf16),
            pltpu.VMEM((devices * qblocks, KEY_BLOCK, 2 * LANES), bf16),
            pltpu.VMEM((count, heads_width), bf16),
            pltpu.VMEM((count, heads_width), bf16),
            pltpu.VMEM((count, heads_width), bf16),
            pltpu.VMEM((out_weight.shape[0], half), bf16),
            pltpu.VMEM((count, half), f32),
            pltpu.VMEM((qblocks, 1, LANES), f32),
            pltpu.VMEM((qblocks, 1, LANES), f32),
            pltpu.SemaphoreType.DMA((qblocks, devices)),
            pltpu.SemaphoreType.DMA((qblocks, devices)),
            pltpu.SemaphoreType.DMA((2,)),
            pltpu.SemaphoreType.DMA((qblocks,)),
            pltpu.SemaphoreType.DMA((qblocks,)),
            pltpu.SemaphoreType.DMA((2,)),
        ],
        compiler_params=pltpu.CompilerParams(
            collective_id=0, has_side_effects=True, vmem_limit_bytes=60 * 1024 * 1024
        ),
    )(
        ids, row_data, query_weight, key_weight, value_weight,
        out_weight, norm_gain[None], far_cos, far_sin,
        jnp.asarray(near_cos), jnp.asarray(near_sin),
    )
    return result[None]


def solution(mesh):
    placed = (
        P("dp", "kv", None),
        P(None, "tp"),
        P(None, "tp"),
        P(None, "tp"),
        P("tp", None),
        P("tp"),
        P("dp", None, None),
        P("dp", None, None),
    )
    return jax.shard_map(
        body, mesh=mesh, in_specs=placed, out_specs=P("dp", "kv", "tp"), check_vma=False
    )
```
